128 devices in a mesh: sp: 16 (over z, x), dp: 8 (over y, core).
Axes of the slice: x: 4, y: 4, z: 4, core: 2. Of those that a mesh axis runs over, the one named last changes fastest.
Arguments:
- skip_stream_entering: bfloat16 [8, 2048, 2048], P('dp', 'sp'), may hold values from -6 to 6
- mapped_probe_matrix: bfloat16 [8, 2048, 2048], P('dp', 'sp'), may hold values from -6 to 6
- mapped_lookup_matrix: bfloat16 [8, 2048, 2048], P('dp', 'sp'), may hold values from -6 to 6
- mapped_content_matrix: bfloat16 [8, 2048, 4096], P('dp', 'sp'), may hold values from -6 to 6
- retention_preactivation: bfloat16 [8, 2048, 2048], P('dp', 'sp'), may hold values from -4 to 12
- extra_shrinkage: float32 [8, 16, 2048], P('dp', 'sp'), may hold values from -0.6932 to 0
- attention_group_scale: float32 [4096], replicated, may hold values from 0.1 to 1.9
- final_projection_matrix: bfloat16 [4096, 2048], P(None, 'dp'), may hold values from -0.09375 to 0.09375
- blender_branch_scale: float32 [2048], replicated, may hold values from 0.1 to 1.9
- specialist_prenormal_scale: float32 [2048], replicated, may hold values from 0.1 to 1.9
- specialist_switch_matrix: bfloat16 [128, 2048, 1024], P(('sp', 'dp')), may hold values from -0.125 to 0.125
- specialist_expand_matrix: bfloat16 [128, 2048, 1024], P(('sp', 'dp')), may hold values from -0.125 to 0.125
- specialist_contract_matrix: bfloat16 [128, 1024, 2048], P(('sp', 'dp')), may hold values from -0.1875 to 0.1875
- specialist_branch_scale: float32 [2048], replicated, may hold values from 0.1 to 1.9
- assigned_specialists: int32 [8, 2048, 2], P('dp', 'sp'), may hold values from 0 to 127, all different within a row; in each aligned block of 128 rows (0 to 127, 128 to 255, ..., all dimensions but the last counted through in order) at most 3 rows name the same one
- dispatcher_logits: float32 [8, 2048, 2], P('dp', 'sp'), may hold values from 0.2 to 1
Outputs:
- layer_out: bfloat16 [8, 2048, 2048], P('dp', 'sp')
The draws below stay inside these ranges and needn't reach their ends.
Inputs may be any that keep to these rules, and one draw needn't show every extreme that they name: `assigned_specialists`: in the rows of one device no expert is named more than 3 times; in every draw some expert reaches 3 on some device.
All inputs are finite; a program needn't handle non-finite values.
Results may differ from the reference program's by a relative error of at most 0.013.
Values may be sent and summed in bfloat16 or wider, within the bound.
No kernel may reach another device: no remote copies, remote signals or barrier semaphores. Data moves between devices by JAX's collectives and lax.ppermute only.
A program may use at most 128 MiB of HBM per device.

```python
import math
import jax
import jax.numpy as jnp
import numpy as np
from jax import lax

D = 2048
ATTENTION_GROUPS = 16
KEY_WIDTH = 128
DV = 256
FF = 1024
TOP = 2
BLOCK = 64
TOK_DEV = 128
BATCH_SAMPLES = 8
TIME_STEPS = 2048
EXPERTS = 128
CAP = 3


def draw_retention_preactivation(key, part):
    kinds = jax.random.randint(jax.random.fold_in(key, 11), (ATTENTION_GROUPS,), 0, 10)
    slowness = (kinds >= 5).astype(jnp.float32)
    slow_center = math.log(TIME_STEPS / 24.0)
    centers = slowness * slow_center + (1.0 - slowness) * 0.5
    channel = jax.random.uniform(jax.random.fold_in(key, 12), (ATTENTION_GROUPS, KEY_WIDTH), jnp.float32, -0.5, 0.5)
    base_rate = (centers[:, None] + channel).reshape(ATTENTION_GROUPS * KEY_WIDTH)
    span_count = TIME_STEPS // TOK_DEV
    shifts = jax.random.uniform(jax.random.fold_in(key, 13), (BATCH_SAMPLES, span_count), jnp.float32, -0.7, 0.7)
    shifts = jnp.repeat(shifts, TOK_DEV, axis=1)
    jitter = 0.8 * jax.random.normal(jax.random.fold_in(key, 14), (BATCH_SAMPLES, TIME_STEPS, ATTENTION_GROUPS * KEY_WIDTH), jnp.float32)
    total = base_rate[None, None, :] + shifts[:, :, None] + jitter
    return jnp.clip(total, -4.0, 12.0).astype(jnp.bfloat16)


def draw_extra_shrinkage(key, part):
    spike_amount = 6
    timestep_offset = jax.random.randint(jax.random.fold_in(key, 21), (BATCH_SAMPLES, ATTENTION_GROUPS, spike_amount), 0, TIME_STEPS)
    tier_amount = jax.random.uniform(jax.random.fold_in(key, 22), (BATCH_SAMPLES, ATTENTION_GROUPS, spike_amount), jnp.float32, math.log(0.5), math.log(0.8))
    places = jnp.arange(TIME_STEPS, dtype=jnp.int32)
    matched = places[None, None, :, None] == timestep_offset[:, :, None, :]
    return jnp.min(jnp.where(matched, tier_amount[:, :, None, :], 0.0), axis=3)


def block_scale(key, dims, split, low, high):
    level = 1.0
    for dim, blocks in split:
        draws = jax.random.uniform(jax.random.fold_in(jax.random.fold_in(key, 6), dim), (blocks,), jnp.float32, low / len(split), high / len(split))
        level = level * jnp.repeat(jnp.exp(draws), dims[dim] // blocks).reshape((-1,) + (1,) * (len(dims) - 1 - dim))
    return level


def assign_block(stream_key, own, number, rows, number_of, top, bound, skew):
    order = jax.random.permutation(stream_key, number_of)
    packed, common = portions_of(number_of, rows * top, bound, skew, True), portions_of(number_of, rows * top, bound, skew, False)
    places = jnp.arange(number_of)

    def named(lengths, rotation):
        used = int((lengths > 0).sum())
        fixed = max(1, used // 4)
        shifted = fixed + (places - fixed + rotation * (used - fixed)) % max(1, number_of - fixed)
        return jnp.zeros((number_of,), jnp.int32).at[order[jnp.where(places < fixed, places, shifted)]].set(jnp.asarray(lengths, jnp.int32))

    lengths = jnp.where(number % 4 == 0, named(packed, number // 4), named(common, number - number // 4 - 1))
    mixed = jax.random.permutation(jax.random.fold_in(own, 3), number_of)
    donor, taker = mixed[0:number_of // 2 * 2:2], mixed[1:number_of // 2 * 2:2]
    room = jnp.minimum(lengths[donor] - 1, bound - lengths[taker]) // 2
    room = jnp.where((donor == order[0]) | (taker == order[0]) | (lengths[taker] == 0), 0, jnp.maximum(room, 0))
    shifted = jax.random.randint(jax.random.fold_in(own, 4), (number_of // 2,), 0, 1 << 20) % (room + 1)
    lengths = lengths.at[donor].add(-shifted).at[taker].add(shifted)
    members = jnp.searchsorted(jnp.cumsum(lengths), jnp.arange(rows * top), side="right").astype(jnp.int32)
    listing = members.reshape(top, rows).T
    listing = listing[jax.random.permutation(jax.random.fold_in(own, 1), rows)]
    rotation = jax.random.randint(jax.random.fold_in(own, 2), (rows, 1), 0, top)
    return jnp.take_along_axis(listing, (jnp.arange(top)[None, :] + rotation) % top, axis=1)


def portions_of(amount, total, bound, slope, full):
    weights = [(1 << 20) // math.isqrt(rank ** slope) + 1 for rank in range(1, amount + 1)]
    largest = bound if full else min(bound, max(-(-total // amount), total * weights[0] // sum(weights)))
    least = 1 if total - largest >= amount - 1 else 0
    holding, surplus = [largest] + [least] * (amount - 1), total - largest - least * (amount - 1)
    while surplus > 0:
        free = [i for i in range(1, amount) if holding[i] < largest] or [i for i in range(1, amount) if holding[i] < bound]
        whole, budget = sum([weights[i] for i in free]), surplus
        for i in free:
            extra = min(bound - holding[i], max(1, budget * weights[i] // whole), surplus)
            holding[i] = holding[i] + extra
            surplus = surplus - extra
    return np.array(holding)


def centred(own_key, shape, scale, limit, split=(), kind=jnp.bfloat16):
    drawn = jax.random.normal(own_key, shape, jnp.float32) * scale
    if len(split) > 0:
        drawn = block_scale(own_key, shape, split, -0.22, 0.18) * drawn
    return jnp.clip(drawn, min=-limit, max=limit).astype(kind)


def setup_inputs(seed: int = 0) -> dict:
    key_list = jax.random.split(jax.random.key(seed), 17)
    skip_stream_entering = centred(key_list[0], (BATCH_SAMPLES, TIME_STEPS, D), 1.0, 6.0, ((0, 8), (1, 16)))
    mapped_probe_matrix = centred(key_list[1], (BATCH_SAMPLES, TIME_STEPS, ATTENTION_GROUPS * KEY_WIDTH), 1.0, 6.0, ((0, 8), (1, 16)))
    mapped_lookup_matrix = centred(key_list[2], (BATCH_SAMPLES, TIME_STEPS, ATTENTION_GROUPS * KEY_WIDTH), 1.0, 6.0, ((0, 8), (1, 16)))
    mapped_content_matrix = centred(key_list[3], (BATCH_SAMPLES, TIME_STEPS, ATTENTION_GROUPS * DV), 1.0, 6.0, ((0, 8), (1, 16)))
    retention_preactivation = draw_retention_preactivation(jax.random.fold_in(key_list[16], 71), 0)
    extra_shrinkage = draw_extra_shrinkage(jax.random.fold_in(key_list[16], 71), 0)
    attention_group_scale = jnp.clip(1.0 + 0.18 * jax.random.normal(key_list[6], (ATTENTION_GROUPS * DV,), jnp.float32), 0.1, 1.9)
    final_projection_matrix = centred(key_list[7], (ATTENTION_GROUPS * DV, D), (ATTENTION_GROUPS * DV) ** -0.5, 0.09375, ((1, 8),))
    blender_branch_scale = jnp.clip(1.0 + 0.18 * jax.random.normal(key_list[8], (D,), jnp.float32), 0.1, 1.9)
    specialist_prenormal_scale = jnp.clip(1.0 + 0.18 * jax.random.normal(key_list[9], (D,), jnp.float32), 0.1, 1.9)
    specialist_switch_matrix = centred(key_list[10], (EXPERTS, D, FF), D ** -0.5, 0.125, ((0, 128),))
    specialist_expand_matrix = centred(key_list[11], (EXPERTS, D, FF), D ** -0.5, 0.125, ((0, 128),))
    specialist_contract_matrix = centred(key_list[12], (EXPERTS, FF, D), FF ** -0.5, 0.1875, ((0, 128),))
    specialist_branch_scale = jnp.clip(1.0 + 0.18 * jax.random.normal(key_list[13], (D,), jnp.float32), 0.1, 1.9)
    assigned_specialists_keys = jax.random.split(jax.random.fold_in(key_list[14], 1), BATCH_SAMPLES * TIME_STEPS // TOK_DEV)
    assigned_specialists_turns = jax.random.permutation(jax.random.fold_in(key_list[14], 3), BATCH_SAMPLES * TIME_STEPS // TOK_DEV)
    assigned_specialists = jax.vmap(lambda own, number: assign_block(jax.random.fold_in(key_list[14], 2), own, number, TOK_DEV, EXPERTS, TOP, CAP, 2))(assigned_specialists_keys, assigned_specialists_turns).reshape((BATCH_SAMPLES, TIME_STEPS, TOP))
    dispatcher_logits = jnp.clip(jnp.exp(math.log(1.0) - 1.609438 * jax.random.uniform(key_list[15], (BATCH_SAMPLES, TIME_STEPS, TOP), jnp.float32) ** block_scale(key_list[15], (BATCH_SAMPLES, TIME_STEPS, TOP), ((0, 8), (1, 16)), -0.2, 0.2)), 0.2, 1.0)
    return dict(skip_stream_entering=skip_stream_entering, mapped_probe_matrix=mapped_probe_matrix, mapped_lookup_matrix=mapped_lookup_matrix, mapped_content_matrix=mapped_content_matrix, retention_preactivation=retention_preactivation, extra_shrinkage=extra_shrinkage, attention_group_scale=attention_group_scale, final_projection_matrix=final_projection_matrix, blender_branch_scale=blender_branch_scale, specialist_prenormal_scale=specialist_prenormal_scale, specialist_switch_matrix=specialist_switch_matrix, specialist_expand_matrix=specialist_expand_matrix, specialist_contract_matrix=specialist_contract_matrix, specialist_branch_scale=specialist_branch_scale, assigned_specialists=assigned_specialists, dispatcher_logits=dispatcher_logits)


epsilon = 1e-06
softness_factor = 16.0
highest = lax.Precision.HIGHEST

def rms_scale(values, gain):
    mean_square = lax.optimization_barrier(jnp.mean(values * values, axis=-1, keepdims=True))
    return values * lax.rsqrt(mean_square + epsilon) * gain

def combine_states(earlier, later):
    return (earlier[0] * later[0], later[0][..., None] * earlier[1] + later[1])

def block_attention(query_f, key_f, value_f, shrink_exponent):
    length_value, head_count, key_dim = query_f.shape
    value_dim = value_f.shape[-1]
    block_count = length_value // BLOCK
    query_blocks = query_f.reshape(block_count, BLOCK, head_count, key_dim)
    key_blocks = key_f.reshape(block_count, BLOCK, head_count, key_dim)
    value_blocks = value_f.reshape(block_count, BLOCK, head_count, value_dim)
    within = jnp.cumsum(shrink_exponent.reshape(block_count, BLOCK, head_count, key_dim), axis=1)
    block_end = within[:, -1]
    lifted = query_blocks * jnp.exp(within)
    lowered = key_blocks * jnp.exp(-within)
    scores = jnp.einsum('nthk,nshk->nhts', lifted, lowered, precision=highest)
    causal = jnp.arange(BLOCK)[:, None] >= jnp.arange(BLOCK)[None, :]
    scores = jnp.where(causal, scores, 0.0)
    inside = jnp.einsum('nhts,nshv->nthv', scores, value_blocks, precision=highest)
    carried_keys = key_blocks * jnp.exp(block_end[:, None] - within)
    updates = jnp.einsum('nshk,nshv->nhkv', carried_keys, value_blocks, precision=highest)
    decays = jnp.exp(block_end)
    total_decay, states = lax.associative_scan(combine_states, (decays, updates), axis=0)
    entering = jnp.concatenate([jnp.zeros_like(states[:1]), states[:-1]], axis=0)
    across = jnp.einsum('nthk,nhkv->nthv', lifted, entering, precision=highest)
    outputs = (inside + across).reshape(length_value, head_count, value_dim)
    offsets = jnp.cumsum(block_end, axis=0) - block_end
    reached = (query_blocks * jnp.exp(within + offsets[:, None])).reshape(length_value, head_count, key_dim)
    return (outputs, total_decay[-1], states[-1], reached)

def reference(skip_stream_entering, mapped_probe_matrix, mapped_lookup_matrix, mapped_content_matrix, retention_preactivation, extra_shrinkage, attention_group_scale, final_projection_matrix, blender_branch_scale, specialist_prenormal_scale, specialist_switch_matrix, specialist_expand_matrix, specialist_contract_matrix, specialist_branch_scale, assigned_specialists, dispatcher_logits):

    def lone_series(fragment_array):
        probe_series, lookup_series, content_series, shrink_series, spike_series = fragment_array
        length_value = probe_series.shape[0]
        query_f = probe_series.reshape(length_value, ATTENTION_GROUPS, KEY_WIDTH).astype(jnp.float32) * KEY_WIDTH ** (-0.5)
        key_f = lookup_series.reshape(length_value, ATTENTION_GROUPS, KEY_WIDTH).astype(jnp.float32)
        value_f = content_series.reshape(length_value, ATTENTION_GROUPS, DV).astype(jnp.float32)
        shrink_exponent = jax.nn.log_sigmoid(shrink_series.reshape(length_value, ATTENTION_GROUPS, KEY_WIDTH).astype(jnp.float32)) / softness_factor
        shrink_exponent = shrink_exponent + jnp.transpose(spike_series)[:, :, None]
        outputs = block_attention(query_f, key_f, value_f, shrink_exponent)[0]
        return rms_scale(outputs, attention_group_scale.reshape(ATTENTION_GROUPS, DV)).astype(jnp.bfloat16)
    attention_group_result = lax.map(lone_series, (mapped_probe_matrix, mapped_lookup_matrix, mapped_content_matrix, retention_preactivation, extra_shrinkage))
    token_count = BATCH_SAMPLES * TIME_STEPS
    attention_group_result = attention_group_result.reshape(token_count, ATTENTION_GROUPS * DV)
    projected = jnp.dot(attention_group_result, final_projection_matrix, preferred_element_type=jnp.float32).astype(jnp.bfloat16)
    stream = skip_stream_entering.reshape(token_count, D).astype(jnp.float32)
    residual = (stream + rms_scale(projected.astype(jnp.float32), blender_branch_scale)).astype(jnp.bfloat16)
    expert_in = rms_scale(residual.astype(jnp.float32), specialist_prenormal_scale).astype(jnp.bfloat16)
    block_total = token_count // TOK_DEV
    pair_dev = TOK_DEV * TOP
    pair_count = token_count * TOP
    chosen = assigned_specialists.reshape(block_total, pair_dev)
    onehot = (chosen[:, :, None] == jnp.arange(EXPERTS, dtype=jnp.int32)[None, None, :]).astype(jnp.int32)
    ranks = lax.optimization_barrier(jnp.sum((jnp.cumsum(onehot, axis=1) - onehot) * onehot, axis=2))
    block_ids = jnp.arange(block_total, dtype=jnp.int32)[:, None]
    slots = (chosen * block_total + block_ids) * CAP + ranks
    pair_ids = jnp.arange(pair_count, dtype=jnp.int32)
    table = jnp.full((EXPERTS * block_total * CAP,), pair_count, jnp.int32)
    table = table.at[slots.reshape(-1)].set(pair_ids).reshape(EXPERTS, block_total * CAP)
    padded = jnp.concatenate([expert_in, jnp.zeros((1, D), jnp.bfloat16)], axis=0)

    def expert_step(carry, fragment_array):
        sources, gate_weight, up_weight, down_weight = fragment_array
        row_block = padded[sources // TOP]
        gate_part = jnp.dot(row_block, gate_weight, preferred_element_type=jnp.float32)
        up_part = jnp.dot(row_block, up_weight, preferred_element_type=jnp.float32)
        hidden_units = (jax.nn.silu(gate_part) * up_part).astype(jnp.bfloat16)
        result = jnp.dot(hidden_units, down_weight, preferred_element_type=jnp.float32).astype(jnp.bfloat16)
        return (carry.at[sources].set(result, mode='drop'), None)
    pair_out, _ = lax.scan(expert_step, jnp.zeros((pair_count, D), jnp.bfloat16), (table, specialist_switch_matrix, specialist_expand_matrix, specialist_contract_matrix))
    weights = dispatcher_logits.reshape(token_count, TOP)
    weights = weights / lax.optimization_barrier(jnp.sum(weights, axis=1, keepdims=True))
    combined = lax.optimization_barrier(jnp.sum(pair_out.reshape(token_count, TOP, D).astype(jnp.float32) * weights[:, :, None], axis=1))
    layer_out = residual.astype(jnp.float32) + rms_scale(combined, specialist_branch_scale)
    return layer_out.astype(jnp.bfloat16).reshape(BATCH_SAMPLES, TIME_STEPS, D)
```

```python
import jax
import jax.numpy as jnp
from jax import lax
from jax.experimental import pallas as pl
from jax.experimental.pallas import tpu as pltpu
from jax.sharding import PartitionSpec as P

D = 2048
HEADS = 16
DK = 128
DV = 256
TOP = 2
CAP = 3
TOK = 128
FF = 1024
EXTRA_ROWS = 8

EPS = 1e-06
F32 = jnp.float32
BF16 = jnp.bfloat16

NN = (((1,), (0,)), ((), ()))
NT = (((1,), (1,)), ((), ()))
TN = (((0,), (0,)), ((), ()))


def mm(a, b, dims=NN):
    return lax.dot_general(a, b, dims, preferred_element_type=F32)


def params(mib=48):
    return pltpu.CompilerParams(vmem_limit_bytes=mib * 2**20)


def cost(flops, nbytes, trans=0):
    return pl.CostEstimate(flops=flops, bytes_accessed=nbytes, transcendentals=trans)


def lower_ones(n):
    return (
        lax.broadcasted_iota(jnp.int32, (n, n), 0) >= lax.broadcasted_iota(jnp.int32, (n, n), 1)
    )


def three_parts(x):
    a = x.astype(BF16)
    r = x - a.astype(F32)
    b = r.astype(BF16)
    c = (r - b.astype(F32)).astype(BF16)
    return a, b, c


def extra_sums(ex):
    low = lower_ones(TOK).astype(BF16)
    parts = three_parts(ex)
    rows = sum(mm(p, low, NT) for p in parts)
    cols = sum(mm(low, p, NT) for p in parts)
    return rows, cols


def prep_kernel(q_ref, k_ref, g_ref, qd_ref, kd_ref, p_ref, bend_ref):
    x = g_ref[...].astype(F32)
    ls = (jnp.minimum(x, 0.0) - jnp.log1p(jnp.exp(-jnp.abs(x)))) * (1.0 / 16.0)
    low = lower_ones(TOK).astype(BF16)
    hi = ls.astype(BF16)
    lo = (ls - hi.astype(F32)).astype(BF16)
    b = mm(low, hi) + mm(low, lo)
    end = b[TOK - 1 : TOK, :]
    k = k_ref[...].astype(F32)
    qd = (q_ref[...].astype(F32) * (DK**-0.5) * jnp.exp(b)).astype(BF16)
    kp = (k * jnp.exp(-b)).astype(BF16)
    qd_ref[...] = qd
    kd_ref[...] = k * jnp.exp(end - b)
    bend_ref[...] = end
    for h in range(p_ref.shape[0]):
        at = slice(h * DK, (h + 1) * DK)
        p_ref[h] = mm(qd[:, at], kp[:, at], NT)


def prep(q, k, g):
    step = 4
    wide = pl.BlockSpec((TOK, step * DK), lambda i: (0, i))
    return pl.pallas_call(
        prep_kernel,
        grid=(HEADS // step,),
        in_specs=[wide, wide, wide],
        out_specs=[
            wide,
            wide,
            pl.BlockSpec((step, TOK, TOK), lambda i: (i, 0, 0)),
            pl.BlockSpec((1, step * DK), lambda i: (0, i)),
        ],
        out_shape=[
            jax.ShapeDtypeStruct((TOK, HEADS * DK), BF16),
            jax.ShapeDtypeStruct((TOK, HEADS * DK), F32),
            jax.ShapeDtypeStruct((HEADS, TOK, TOK), F32),
            jax.ShapeDtypeStruct((1, HEADS * DK), F32),
        ],
        compiler_params=params(),
        cost_estimate=cost(2 * 10**9, 4 * 2**20, 2**20),
        name="prep",
    )(q, k, g)


def update_kernel(ex_ref, kd_ref, v_ref, bend_ref, u_ref):
    rows, cols = extra_sums(ex_ref[...])
    w = jnp.exp(cols[TOK - 1 : TOK, :] - cols)
    for h in range(HEADS):
        kd = (kd_ref[:, h * DK : (h + 1) * DK] * w[:, h : h + 1]).astype(BF16)
        u = mm(kd, v_ref[:, h * DV : (h + 1) * DV], TN)
        u_ref[h, 0:DK, :] = u.astype(BF16)
        end = bend_ref[:, h * DK : (h + 1) * DK] + rows[h : h + 1, TOK - 1 : TOK]
        hi = end.astype(BF16)
        lo = (end - hi.astype(F32)).astype(BF16)
        both = jnp.concatenate([hi.astype(F32), lo.astype(F32)], axis=1)
        u_ref[h, DK : DK + EXTRA_ROWS, :] = jnp.broadcast_to(both, (EXTRA_ROWS, DV)).astype(BF16)


def update(ex, kd, v, bend):
    return pl.pallas_call(
        update_kernel,
        out_shape=jax.ShapeDtypeStruct((HEADS, DK + EXTRA_ROWS, DV), BF16),
        compiler_params=params(),
        cost_estimate=cost(2 * 10**9, 3 * 2**20),
        name="update",
    )(ex, kd, v, bend)


def inside_kernel(ex_ref, p_ref, v_ref, o_ref):
    rows, cols = extra_sums(ex_ref[...])
    keep = lower_ones(TOK)
    for h in range(HEADS):
        gap = jnp.minimum(cols[:, h : h + 1] - rows[h : h + 1, :], 0.0)
        a = jnp.where(keep, p_ref[h] * jnp.exp(gap), 0.0).astype(BF16)
        o_ref[:, h * DV : (h + 1) * DV] = mm(a, v_ref[:, h * DV : (h + 1) * DV])


def inside(ex, p, v):
    return pl.pallas_call(
        inside_kernel,
        out_shape=jax.ShapeDtypeStruct((TOK, HEADS * DV), F32),
        compiler_params=params(),
        cost_estimate=cost(4 * 10**9, 4 * 2**20, 2**18),
        name="inside",
    )(ex, p, v)


def prefix_kernel(u_ref, s_ref):
    chunks = u_ref.shape[0]
    tail = u_ref[:, DK : DK + EXTRA_ROWS, :].astype(F32)
    ends = tail[:, 0, 0:DK] + tail[:, 0, DK : 2 * DK]
    keep = jnp.transpose(jnp.exp(ends))
    state = jnp.zeros((DK, DV), F32)
    for m in range(chunks):
        s_ref[m] = state.astype(BF16)
        if m + 1 < chunks:
            state = state * keep[:, m : m + 1] + u_ref[m, 0:DK, :].astype(F32)


def prefix(u):
    return pl.pallas_call(
        prefix_kernel,
        out_shape=jax.ShapeDtypeStruct((u.shape[0], DK, DV), BF16),
        compiler_params=params(),
        cost_estimate=cost(10**8, 2 * 2**20),
        name="prefix",
    )(u)


def heads_kernel(ex_ref, qd_ref, s_ref, o_ref, gain_ref, out_ref):
    _, cols = extra_sums(ex_ref[...])
    grow = jnp.exp(cols)
    for h in range(HEADS):
        at = slice(h * DV, (h + 1) * DV)
        cross = mm(qd_ref[:, h * DK : (h + 1) * DK], s_ref[h])
        o = o_ref[:, at] + cross * grow[:, h : h + 1]
        ms = jnp.mean(o * o, axis=1, keepdims=True)
        out_ref[:, at] = (o * lax.rsqrt(ms + EPS) * gain_ref[:, at]).astype(BF16)


def heads(ex, qd, s, o, gain):
    return pl.pallas_call(
        heads_kernel,
        out_shape=jax.ShapeDtypeStruct((TOK, HEADS * DV), BF16),
        compiler_params=params(),
        cost_estimate=cost(2 * 10**9, 5 * 2**20),
        name="heads",
    )(ex, qd, s, o, gain)


KB = 512


def early_kernel(x_ref, *refs):
    n = (len(refs) - 2)
    w_refs, out_ref, acc_ref = refs[:n], refs[n], refs[n + 1]
    i = pl.program_id(0)

    @pl.when(i == 0)
    def _():
        acc_ref[...] = jnp.zeros_like(acc_ref)

    x = x_ref[...]
    for p in range(n):
        acc_ref[p] += mm(x, w_refs[p][...])

    @pl.when(i == pl.num_programs(0) - 1)
    def _():
        out_ref[...] = acc_ref[...].astype(BF16)


def early(x, ws):
    n = len(ws)
    depth, wide = ws[0].shape
    return pl.pallas_call(
        early_kernel,
        grid=(depth // KB,),
        in_specs=[pl.BlockSpec((TOK, KB), lambda i: (0, i))]
        + [pl.BlockSpec((KB, wide), lambda i: (i, 0))] * n,
        out_specs=pl.BlockSpec((n, TOK, wide), lambda i: (0, 0, 0)),
        out_shape=jax.ShapeDtypeStruct((n, TOK, wide), BF16),
        scratch_shapes=[pltpu.VMEM((n, TOK, wide), F32)],
        compiler_params=params(),
        cost_estimate=cost(2 * TOK * depth * wide * n, 2 * depth * wide * n),
        name="early",
    )(x, *ws)


def late_kernel(place_ref, x_ref, *refs):
    done_ref, skip_ref, g1_ref, g2_ref = refs[0:4]
    res_ref, ein_ref, acc_ref, proj_ref = refs[-4:]
    w_refs = refs[4:-4]
    n = len(w_refs)
    i = pl.program_id(0)

    @pl.when(i == 0)
    def _():
        acc_ref[...] = jnp.zeros_like(acc_ref)

    x = x_ref[...]
    for p in range(n):
        acc_ref[p] += mm(x, w_refs[p][...])

    @pl.when(i == pl.num_programs(0) - 1)
    def _():
        m = done_ref.shape[0]
        for p in range(m):
            proj_ref[place_ref[p]] = done_ref[p].astype(F32)
        for p in range(n):
            proj_ref[place_ref[m + p]] = acc_ref[p].astype(BF16).astype(F32)
        wide = proj_ref.shape[2]
        ms = jnp.zeros((TOK, 1), F32)
        for d in range(m + n):
            pr = proj_ref[d]
            ms += jnp.sum(pr * pr, axis=1, keepdims=True)
        inv = lax.rsqrt(ms * (1.0 / D) + EPS)
        ms = jnp.zeros((TOK, 1), F32)
        for d in range(m + n):
            at = slice(d * wide, (d + 1) * wide)
            r = (skip_ref[:, at].astype(F32) + proj_ref[d] * inv * g1_ref[:, at]).astype(BF16)
            res_ref[:, at] = r
            rf = r.astype(F32)
            proj_ref[d] = rf
            ms += jnp.sum(rf * rf, axis=1, keepdims=True)
        inv = lax.rsqrt(ms * (1.0 / D) + EPS)
        for d in range(m + n):
            at = slice(d * wide, (d + 1) * wide)
            ein_ref[:, at] = (proj_ref[d] * inv * g2_ref[:, at]).astype(BF16)


def late(place, x, done, skip, g1, g2, ws):
    n = len(ws)
    depth, wide = ws[0].shape
    whole2 = lambda i: (0, 0)
    return pl.pallas_call(
        late_kernel,
        grid=(depth // KB,),
        in_specs=[
            pl.BlockSpec(memory_space=pltpu.SMEM),
            pl.BlockSpec((TOK, KB), lambda i: (0, i)),
            pl.BlockSpec(done.shape, lambda i: (0, 0, 0)),
            pl.BlockSpec((TOK, D), whole2),
            pl.BlockSpec((1, D), whole2),
            pl.BlockSpec((1, D), whole2),
        ]
        + [pl.BlockSpec((KB, wide), lambda i: (i, 0))] * n,
        out_specs=[pl.BlockSpec((TOK, D), whole2), pl.BlockSpec((TOK, D), whole2)],
        out_shape=[jax.ShapeDtypeStruct((TOK, D), BF16), jax.ShapeDtypeStruct((TOK, D), BF16)],
        scratch_shapes=[
            pltpu.VMEM((n, TOK, wide), F32),
            pltpu.VMEM((D // wide, TOK, wide), F32),
        ],
        compiler_params=params(),
        cost_estimate=cost(2 * TOK * depth * wide * n, 2 * depth * wide * n),
        name="late",
    )(place, x, done, skip, g1, g2, *ws)


def send_kernel(slot_ref, x_ref, out_ref):
    out_ref[...] = jnp.zeros_like(out_ref)

    def body(t, _):
        row = x_ref[t]
        out_ref[slot_ref[TOP * t]] = row
        out_ref[slot_ref[TOP * t + 1]] = row
        return 0

    lax.fori_loop(0, TOK, body, 0, unroll=8)


def send_rows(slots, x3, rows):
    return pl.pallas_call(
        send_kernel,
        in_specs=[
            pl.BlockSpec(memory_space=pltpu.SMEM),
            pl.BlockSpec(memory_space=pltpu.VMEM),
        ],
        out_shape=jax.ShapeDtypeStruct((rows, 16, 128), BF16),
        compiler_params=params(),
        cost_estimate=cost(10**6, 2 * 2**20),
        name="send_rows",
    )(slots, x3)


def expert_kernel(x_ref, wg_ref, wu_ref, wd_ref, out_ref, acc_ref):
    i = pl.program_id(0)
    x = x_ref[...]
    gate = mm(x, wg_ref[...])
    up = mm(x, wu_ref[...])
    hid = (gate * jax.nn.sigmoid(gate) * up).astype(BF16)
    part = mm(hid, wd_ref[...])

    @pl.when(i == 0)
    def _():
        acc_ref[...] = part

    @pl.when((i > 0) & (i < pl.num_programs(0) - 1))
    def _():
        acc_ref[...] += part

    @pl.when(i == pl.num_programs(0) - 1)
    def _():
        out_ref[...] = (acc_ref[...] + part).astype(BF16)


def experts(x, wg, wu, wd):
    rows = x.shape[0]
    fb = 256
    return pl.pallas_call(
        expert_kernel,
        grid=(FF // fb,),
        in_specs=[
            pl.BlockSpec((rows, D), lambda i: (0, 0)),
            pl.BlockSpec((D, fb), lambda i: (0, i)),
            pl.BlockSpec((D, fb), lambda i: (0, i)),
            pl.BlockSpec((fb, D), lambda i: (i, 0)),
        ],
        out_specs=pl.BlockSpec((rows, D), lambda i: (0, 0)),
        out_shape=jax.ShapeDtypeStruct((rows, D), BF16),
        scratch_shapes=[pltpu.VMEM((rows, D), F32)],
        compiler_params=params(),
        cost_estimate=cost(6 * rows * D * FF, 6 * D * FF),
        name="experts",
    )(x, wg, wu, wd)


def combine_kernel(slot_ref, w_ref, back_ref, res_ref, gain_ref, out_ref):
    gain = gain_ref[...]

    def body(i, _):
        for j in range(8):
            t = i * 8 + j
            a = back_ref[slot_ref[TOP * t]].astype(F32) * w_ref[TOP * t]
            b = back_ref[slot_ref[TOP * t + 1]].astype(F32) * w_ref[TOP * t + 1]
            c = a + b
            ms = jnp.sum(c * c, keepdims=True).reshape(1, 1) * (1.0 / D)
            out_ref[t] = (res_ref[t].astype(F32) + c * lax.rsqrt(ms + EPS) * gain).astype(BF16)
        return 0

    lax.fori_loop(0, TOK // 8, body, 0)


def combine(slots, weights, back, res3, gain):
    smem = pl.BlockSpec(memory_space=pltpu.SMEM)
    vmem = pl.BlockSpec(memory_space=pltpu.VMEM)
    return pl.pallas_call(
        combine_kernel,
        in_specs=[smem, smem, vmem, vmem, vmem],
        out_shape=jax.ShapeDtypeStruct((TOK, 16, 128), BF16),
        compiler_params=params(),
        cost_estimate=cost(10**7, 3 * 2**20),
        name="combine",
    )(slots, weights, back, res3, gain)


def shards(
    skip_stream_entering,
    mapped_probe_matrix,
    mapped_lookup_matrix,
    mapped_content_matrix,
    retention_preactivation,
    extra_shrinkage,
    attention_group_scale,
    final_projection_matrix,
    blender_branch_scale,
    specialist_prenormal_scale,
    specialist_switch_matrix,
    specialist_expand_matrix,
    specialist_contract_matrix,
    specialist_branch_scale,
    assigned_specialists,
    dispatcher_logits,
):
    sp_count = lax.axis_size("sp")
    dp_count = lax.axis_size("dp")
    total = sp_count * dp_count

    core = lax.axis_index("dp") % 2
    ychip = lax.axis_index("dp") // 2
    ychips = dp_count // 2

    def ring(sign):
        out = []
        for d in range(dp_count):
            y, c = d // 2, d % 2
            s = sign if c == 0 else -sign
            out.append((d, ((y + s) % ychips) * 2 + c))
        return out

    swap = [(d, d ^ 1) for d in range(dp_count)]
    w_own = final_projection_matrix
    w_a = lax.ppermute(w_own, "dp", ring(1))
    w_b = lax.ppermute(w_own, "dp", ring(-1))
    w_own_s = lax.ppermute(w_own, "dp", swap)

    q = mapped_probe_matrix[0]
    k = mapped_lookup_matrix[0]
    v = mapped_content_matrix[0]
    g = retention_preactivation[0]
    ex = lax.all_to_all(
        extra_shrinkage[0].reshape(sp_count, 1, TOK), "sp", split_axis=0, concat_axis=0, tiled=True
    ).reshape(HEADS, TOK)
    qd, kd, p, bend = prep(q, k, g)
    u = update(ex, kd, v, bend)
    u_in = lax.all_to_all(u, "sp", split_axis=0, concat_axis=0, tiled=True)
    o_in = inside(ex, p, v)
    s = prefix(u_in)
    s_in = lax.all_to_all(s, "sp", split_axis=0, concat_axis=0, tiled=True)

    w_a_f, _ = lax.optimization_barrier((w_a, s))
    w_a2 = lax.ppermute(w_a_f, "dp", ring(1))
    w_a_s = lax.ppermute(w_a_f, "dp", swap)
    w_b_s = lax.ppermute(w_b, "dp", swap)
    w_a2_s = lax.ppermute(w_a2, "dp", swap)

    head_out = heads(ex, qd, s_in, o_in, attention_group_scale.reshape(1, HEADS * DV))

    sgn = 1 - 2 * core
    y_a = (ychip - sgn) % ychips
    y_b = (ychip + sgn) % ychips
    y_a2 = (ychip - 2 * sgn) % ychips
    y_as = (ychip + sgn) % ychips
    y_bs = (ychip - sgn) % ychips
    other = 1 - core
    place = jnp.stack(
        [
            ychip * 2 + core,
            ychip * 2 + other,
            y_a * 2 + core,
            y_as * 2 + other,
            y_b * 2 + core,
            y_bs * 2 + other,
            y_a2 * 2 + core,
            y_a2 * 2 + other,
        ]
    ).astype(jnp.int32)
    done = early(head_out, [w_own, w_own_s, w_a, w_a_s, w_b, w_b_s])
    residual, expert_in = late(
        place,
        head_out,
        done,
        skip_stream_entering[0],
        blender_branch_scale.reshape(1, D),
        specialist_prenormal_scale.reshape(1, D),
        [w_a2, w_a2_s],
    )

    chosen = assigned_specialists[0].reshape(-1)
    onehot = (chosen[:, None] == jnp.arange(total, dtype=jnp.int32)[None, :]).astype(jnp.int32)
    ranks = jnp.sum((jnp.cumsum(onehot, axis=0) - onehot) * onehot, axis=1)
    slots = chosen * CAP + ranks
    weights = dispatcher_logits[0]
    weights = (weights / jnp.sum(weights, axis=1, keepdims=True)).reshape(-1)

    outgoing = send_rows(slots, expert_in.reshape(TOK, 16, 128), total * CAP)
    arrived = lax.all_to_all(
        outgoing.reshape(total, CAP, 16, 128),
        ("sp", "dp"),
        split_axis=0,
        concat_axis=0,
        tiled=True,
    )
    result = experts(
        arrived.reshape(total * CAP, D),
        specialist_switch_matrix[0],
        specialist_expand_matrix[0],
        specialist_contract_matrix[0],
    )
    back = lax.all_to_all(
        result.reshape(total, CAP, 16, 128),
        ("sp", "dp"),
        split_axis=0,
        concat_axis=0,
        tiled=True,
    ).reshape(total * CAP, 16, 128)
    out = combine(
        slots,
        weights,
        back,
        residual.reshape(TOK, 16, 128),
        specialist_branch_scale.reshape(16, 128),
    )
    return out.reshape(1, TOK, D)


def solution(mesh):
    return jax.shard_map(
        shards,
        mesh=mesh,
        in_specs=(
            P("dp", "sp", None),
            P("dp", "sp", None),
            P("dp", "sp", None),
            P("dp", "sp", None),
            P("dp", "sp", None),
            P("dp", "sp", None),
            P(),
            P(None, "dp"),
            P(),
            P(),
            P(("sp", "dp"), None, None),
            P(("sp", "dp"), None, None),
            P(("sp", "dp"), None, None),
            P(),
            P("dp", "sp", None),
            P("dp", "sp", None),
        ),
        out_specs=P("dp", "sp", None),
        check_vma=False,
    )
```

```python
import jax
import jax.numpy as jnp
from jax import lax
from jax.experimental import pallas as pl
from jax.experimental.pallas import tpu as pltpu
from jax.sharding import PartitionSpec as P


D = 2048
HEADS = 16
DK = 128
DV = 256
TOP = 2
CAP = 3
TOK = 128
FF = 1024
EXTRA_ROWS = 8

EPS = 1e-06
F32 = jnp.float32
BF16 = jnp.bfloat16

NN = (((1,), (0,)), ((), ()))
NT = (((1,), (1,)), ((), ()))
TN = (((0,), (0,)), ((), ()))


def mm(a, b, dims=NN):
    return lax.dot_general(a, b, dims, preferred_element_type=F32)


def params(mib):
    return pltpu.CompilerParams(vmem_limit_bytes=mib * 2**20)


def cost(flops, nbytes, trans=0):
    return pl.CostEstimate(flops=flops, bytes_accessed=nbytes, transcendentals=trans)


def lower_ones(n):
    return (
        lax.broadcasted_iota(jnp.int32, (n, n), 0) >= lax.broadcasted_iota(jnp.int32, (n, n), 1)
    )


def three_parts(x):
    a = x.astype(BF16)
    r = x - a.astype(F32)
    b = r.astype(BF16)
    c = (r - b.astype(F32)).astype(BF16)
    return a, b, c


def extra_sums(ex):
    low = lower_ones(TOK).astype(BF16)
    parts = three_parts(ex)
    rows = sum(mm(p, low, NT) for p in parts)
    cols = sum(mm(low, p, NT) for p in parts)
    return rows, cols


def prep_kernel(q_hbm, k_hbm, g_hbm, qd_ref, kd_ref, p_ref, bend_ref, q_ref, k_ref, g_ref, sems):
    parts = 4
    wide = HEADS * DK // parts
    low = lower_ones(TOK).astype(BF16)

    def moves(i):
        at = slice(i * wide, (i + 1) * wide)
        return [
            pltpu.make_async_copy(src.at[:, at], dst.at[:, at], sems.at[i, n])
            for n, (src, dst) in enumerate(((g_hbm, g_ref), (k_hbm, k_ref), (q_hbm, q_ref)))
        ]

    for i in range(parts):
        for m in moves(i):
            m.start()
    for i in range(parts):
        for m in moves(i):
            m.wait()
        at = slice(i * wide, (i + 1) * wide)
        x = g_ref[:, at].astype(F32)
        ls = (jnp.minimum(x, 0.0) - jnp.log1p(jnp.exp(-jnp.abs(x)))) * (1.0 / 16.0)
        hi = ls.astype(BF16)
        lo = (ls - hi.astype(F32)).astype(BF16)
        b = mm(low, hi) + mm(low, lo)
        end = b[TOK - 1 : TOK, :]
        k = k_ref[:, at].astype(F32)
        qd = (q_ref[:, at].astype(F32) * (DK**-0.5) * jnp.exp(b)).astype(BF16)
        kp = (k * jnp.exp(-b)).astype(BF16)
        qd_ref[:, at] = qd
        kd_ref[:, at] = (k * jnp.exp(end - b)).astype(BF16)
        bend_ref[:, at] = end
        for j in range(HEADS // parts):
            h = slice(j * DK, (j + 1) * DK)
            p_ref[i * (HEADS // parts) + j] = mm(qd[:, h], kp[:, h], NT).astype(BF16)


def prep(q, k, g):
    hbm = pl.BlockSpec(memory_space=pltpu.HBM)
    return pl.pallas_call(
        prep_kernel,
        in_specs=[hbm, hbm, hbm],
        out_shape=[
            jax.ShapeDtypeStruct((TOK, HEADS * DK), BF16),
            jax.ShapeDtypeStruct((TOK, HEADS * DK), BF16),
            jax.ShapeDtypeStruct((HEADS, TOK, TOK), BF16),
            jax.ShapeDtypeStruct((1, HEADS * DK), F32),
        ],
        scratch_shapes=[pltpu.VMEM((TOK, HEADS * DK), BF16)] * 3
        + [pltpu.SemaphoreType.DMA((4, 3))],
        compiler_params=params(10),
        cost_estimate=cost(2 * 10**9, 4 * 2**20, 2**20),
        name="prep",
    )(q, k, g)


def update_kernel(ex_ref, kd_ref, v_ref, bend_ref, u_ref):
    rows, cols = extra_sums(ex_ref[...])
    w = jnp.exp(cols[TOK - 1 : TOK, :] - cols)
    for h in range(HEADS):
        kd = (kd_ref[:, h * DK : (h + 1) * DK].astype(F32) * w[:, h : h + 1]).astype(BF16)
        u = mm(kd, v_ref[:, h * DV : (h + 1) * DV], TN)
        u_ref[h, 0:DK, :] = u.astype(BF16)
        end = bend_ref[:, h * DK : (h + 1) * DK] + rows[h : h + 1, TOK - 1 : TOK]
        hi = end.astype(BF16)
        lo = (end - hi.astype(F32)).astype(BF16)
        both = jnp.concatenate([hi.astype(F32), lo.astype(F32)], axis=1)
        u_ref[h, DK : DK + EXTRA_ROWS, :] = jnp.broadcast_to(both, (EXTRA_ROWS, DV)).astype(BF16)


def update(ex, kd, v, bend):
    return pl.pallas_call(
        update_kernel,
        out_shape=jax.ShapeDtypeStruct((HEADS, DK + EXTRA_ROWS, DV), BF16),
        compiler_params=params(8),
        cost_estimate=cost(2 * 10**9, 3 * 2**20),
        name="update",
    )(ex, kd, v, bend)


def inside_kernel(ex_ref, p_ref, v_ref, o_ref):
    rows, cols = extra_sums(ex_ref[...])
    keep = lower_ones(TOK)
    for h in range(HEADS):
        gap = jnp.minimum(cols[:, h : h + 1] - rows[h : h + 1, :], 0.0)
        a = jnp.where(keep, p_ref[h].astype(F32) * jnp.exp(gap), 0.0).astype(BF16)
        o_ref[:, h * DV : (h + 1) * DV] = mm(a, v_ref[:, h * DV : (h + 1) * DV]).astype(BF16)


def inside(ex, p, v):
    return pl.pallas_call(
        inside_kernel,
        out_shape=jax.ShapeDtypeStruct((TOK, HEADS * DV), BF16),
        compiler_params=params(10),
        cost_estimate=cost(4 * 10**9, 4 * 2**20, 2**18),
        name="inside",
    )(ex, p, v)


def prefix_kernel(u_ref, s_ref):
    chunks = u_ref.shape[0]
    tail = u_ref[:, DK : DK + EXTRA_ROWS, :].astype(F32)
    ends = tail[:, 0, 0:DK] + tail[:, 0, DK : 2 * DK]
    keep = jnp.transpose(jnp.exp(ends))
    state = jnp.zeros((DK, DV), F32)
    for m in range(chunks):
        s_ref[m] = state.astype(BF16)
        if m + 1 < chunks:
            state = state * keep[:, m : m + 1] + u_ref[m, 0:DK, :].astype(F32)


def prefix(u):
    return pl.pallas_call(
        prefix_kernel,
        out_shape=jax.ShapeDtypeStruct((u.shape[0], DK, DV), BF16),
        compiler_params=params(8),
        cost_estimate=cost(10**8, 2 * 2**20),
        name="prefix",
    )(u)


def heads_kernel(ex_ref, qd_ref, s_ref, o_ref, gain_ref, out_ref):
    _, cols = extra_sums(ex_ref[...])
    grow = jnp.exp(cols)
    for h in range(HEADS):
        at = slice(h * DV, (h + 1) * DV)
        cross = mm(qd_ref[:, h * DK : (h + 1) * DK], s_ref[h])
        o = o_ref[:, at].astype(F32) + cross * grow[:, h : h + 1]
        ms = jnp.mean(o * o, axis=1, keepdims=True)
        out_ref[:, at] = (o * lax.rsqrt(ms + EPS) * gain_ref[:, at]).astype(BF16)


def heads(ex, qd, s, o, gain):
    return pl.pallas_call(
        heads_kernel,
        out_shape=jax.ShapeDtypeStruct((TOK, HEADS * DV), BF16),
        compiler_params=params(10),
        cost_estimate=cost(2 * 10**9, 5 * 2**20),
        name="heads",
    )(ex, qd, s, o, gain)


KB = 1024
EARLY = 17


def early_kernel(x_ref, y_ref, *refs):
    n = len(refs) - 3
    w_hbm, out_ref, w_ref, sems = refs[:n], refs[n], refs[n + 1], refs[n + 2]
    steps = x_ref.shape[1] // KB

    def move(p, i):
        at = slice(i * KB, (i + 1) * KB)
        return pltpu.make_async_copy(w_hbm[p].at[at, :], w_ref.at[p, at, :], sems.at[p, i])

    for p in range(n):
        for i in range(steps):
            move(p, i).start()
    for p in range(n):
        acc = None
        for i in range(steps):
            at = slice(i * KB, (i + 1) * KB)
            move(p, i).wait()
            x = jnp.concatenate([x_ref[:, at], y_ref[:, at]], axis=0)
            part = mm(x, w_ref[p, at, :])
            acc = part if acc is None else acc + part
        out_ref[p] = acc.astype(BF16)


def early(x, y, ws):
    n = len(ws)
    depth, wide = ws[0].shape
    vmem = pl.BlockSpec(memory_space=pltpu.VMEM)
    return pl.pallas_call(
        early_kernel,
        in_specs=[vmem] * 2 + [pl.BlockSpec(memory_space=pltpu.HBM)] * n,
        out_shape=jax.ShapeDtypeStruct((n, 2 * TOK, wide), BF16),
        scratch_shapes=[
            pltpu.VMEM((n, depth, wide), BF16),
            pltpu.SemaphoreType.DMA((n, depth // KB)),
        ],
        compiler_params=params(EARLY),
        cost_estimate=cost(4 * TOK * depth * wide * n, 2 * depth * wide * n),
    )(x, y, *ws)


PITCH = 24
ROW = 16


def route_kernel(
    place_ref,
    slot_ref,
    e_ref,
    l_ref,
    es_ref,
    ls_ref,
    skip_ref,
    g1_ref,
    g2_ref,
    res_ref,
    out_ref,
    proj_ref,
    row_ref,
):
    out_ref[...] = jnp.zeros_like(out_ref)
    n = 0
    for ref in (e_ref, l_ref, es_ref, ls_ref):
        for p in range(ref.shape[0]):
            proj_ref[place_ref[n]] = ref[p, 0:TOK, :].astype(F32)
            n += 1
    wide = proj_ref.shape[2]
    ms = jnp.zeros((TOK, 1), F32)
    for d in range(n):
        pr = proj_ref[d]
        ms += jnp.sum(pr * pr, axis=1, keepdims=True)
    inv = lax.rsqrt(ms * (1.0 / D) + EPS)
    ms = jnp.zeros((TOK, 1), F32)
    for d in range(n):
        at = slice(d * wide, (d + 1) * wide)
        r = (skip_ref[:, at].astype(F32) + proj_ref[d] * inv * g1_ref[:, at]).astype(BF16)
        res_ref[:, at] = r
        rf = r.astype(F32)
        proj_ref[d] = rf
        ms += jnp.sum(rf * rf, axis=1, keepdims=True)
    inv = lax.rsqrt(ms * (1.0 / D) + EPS)
    for d in range(n):
        at = slice(d * wide, (d + 1) * wide)
        ein = proj_ref[d] * inv * g2_ref[:, at]
        for j in range(wide // 128):
            row_ref[pl.ds(d * (wide // 128) + j, TOK, stride=PITCH), :] = ein[
                :, j * 128 : (j + 1) * 128
            ]

    def body(t, _):
        row = row_ref[pl.ds(pl.multiple_of(t * PITCH, 8), ROW), :].astype(BF16)
        out_ref[slot_ref[TOP * t]] = row
        out_ref[slot_ref[TOP * t + 1]] = row
        return 0

    lax.fori_loop(0, TOK, body, 0, unroll=8)


def route(place, slots, e, l, es, ls, skip, g1, g2, rows):
    wide = e.shape[2]
    vmem = pl.BlockSpec(memory_space=pltpu.VMEM)
    return pl.pallas_call(
        route_kernel,
        in_specs=[pl.BlockSpec(memory_space=pltpu.SMEM)] * 2 + [vmem] * 7,
        out_shape=[
            jax.ShapeDtypeStruct((TOK, D), BF16),
            jax.ShapeDtypeStruct((rows, ROW, 128), BF16),
        ],
        scratch_shapes=[
            pltpu.VMEM((D // wide, TOK, wide), F32),
            pltpu.VMEM((TOK * PITCH, 128), F32),
        ],
        compiler_params=params(12),
        cost_estimate=cost(10**8, 3 * 2**20),
        name="route",
    )(place, slots, e, l, es, ls, skip, g1, g2)


def expert_kernel(x_ref, wg_hbm, wu_hbm, wd_hbm, out_ref, wg_ref, wu_ref, wd_ref, hid_ref, sems):
    parts = 4
    fb = FF // parts

    def moves(i):
        at = slice(i * fb, (i + 1) * fb)
        return (
            pltpu.make_async_copy(wg_hbm.at[:, at], wg_ref.at[:, at], sems.at[0, i]),
            pltpu.make_async_copy(wu_hbm.at[:, at], wu_ref.at[:, at], sems.at[1, i]),
            pltpu.make_async_copy(wd_hbm.at[at, :], wd_ref.at[at, :], sems.at[2, i]),
        )

    for n in range(2):
        for i in range(parts):
            for m in moves(i)[0:2] if n == 0 else moves(i)[2:]:
                m.start()
    x = x_ref[...]
    for i in range(parts):
        at = slice(i * fb, (i + 1) * fb)
        for m in moves(i)[0:2]:
            m.wait()
        gate = mm(x, wg_ref[:, at])
        up = mm(x, wu_ref[:, at])
        hid_ref[:, at] = (gate * jax.nn.sigmoid(gate) * up).astype(BF16)
    for i in range(parts):
        moves(i)[2].wait()
    hid = hid_ref[...]
    nb = 512
    for i in range(D // nb):
        at = slice(i * nb, (i + 1) * nb)
        out_ref[:, at] = mm(hid, wd_ref[:, at]).astype(BF16)


def experts(x, wg, wu, wd):
    rows = x.shape[0]
    hbm = pl.BlockSpec(memory_space=pltpu.HBM)
    return pl.pallas_call(
        expert_kernel,
        in_specs=[pl.BlockSpec(memory_space=pltpu.VMEM), hbm, hbm, hbm],
        out_shape=jax.ShapeDtypeStruct((rows, D), BF16),
        scratch_shapes=[
            pltpu.VMEM((D, FF), BF16),
            pltpu.VMEM((D, FF), BF16),
            pltpu.VMEM((FF, D), BF16),
            pltpu.VMEM((rows, FF), BF16),
            pltpu.SemaphoreType.DMA((3, 4)),
        ],
        compiler_params=params(48),
        cost_estimate=cost(6 * rows * D * FF, 6 * D * FF),
        name="experts",
    )(x, wg, wu, wd)


def combine_kernel(slot_ref, w_ref, back_ref, res_ref, gain_ref, out_ref, row_ref, sq_ref):
    def body(i, _):
        for j in range(8):
            t = i * 8 + j
            a = back_ref[slot_ref[TOP * t]].astype(F32) * w_ref[TOP * t]
            b = back_ref[slot_ref[TOP * t + 1]].astype(F32) * w_ref[TOP * t + 1]
            c = a + b
            row_ref[pl.ds(pl.multiple_of(t * PITCH, 8), ROW), :] = c
            sq_ref[pl.ds(t, 1), :] = jnp.sum(c * c, axis=0, keepdims=True)
        return 0

    lax.fori_loop(0, TOK // 8, body, 0)
    ms = jnp.sum(sq_ref[...], axis=1, keepdims=True) * (1.0 / D)
    inv = lax.rsqrt(ms + EPS)
    for j in range(ROW):
        at = slice(j * 128, (j + 1) * 128)
        c = row_ref[pl.ds(j, TOK, stride=PITCH), :]
        out_ref[:, at] = (res_ref[:, at].astype(F32) + c * inv * gain_ref[:, at]).astype(BF16)


def combine(slots, weights, back, res, gain):
    smem = pl.BlockSpec(memory_space=pltpu.SMEM)
    vmem = pl.BlockSpec(memory_space=pltpu.VMEM)
    return pl.pallas_call(
        combine_kernel,
        in_specs=[smem, smem, vmem, vmem, vmem],
        out_shape=jax.ShapeDtypeStruct((TOK, D), BF16),
        scratch_shapes=[pltpu.VMEM((TOK * PITCH, 128), F32), pltpu.VMEM((TOK, 128), F32)],
        compiler_params=params(8),
        cost_estimate=cost(10**7, 3 * 2**20),
        name="combine",
    )(slots, weights, back, res, gain)


def layer(
    skip_stream_entering,
    mapped_probe_matrix,
    mapped_lookup_matrix,
    mapped_content_matrix,
    retention_preactivation,
    extra_shrinkage,
    attention_group_scale,
    final_projection_matrix,
    blender_branch_scale,
    specialist_prenormal_scale,
    specialist_switch_matrix,
    specialist_expand_matrix,
    specialist_contract_matrix,
    specialist_branch_scale,
    assigned_specialists,
    dispatcher_logits,
):
    sp_count = lax.axis_size("sp")
    dp_count = lax.axis_size("dp")
    total = sp_count * dp_count

    core = lax.axis_index("dp") % 2
    ychip = lax.axis_index("dp") // 2
    ychips = dp_count // 2

    def ring(sign):
        out = []
        for d in range(dp_count):
            y, c = d // 2, d % 2
            s = sign if c == 0 else -sign
            out.append((d, ((y + s) % ychips) * 2 + c))
        return out

    swap = [(d, d ^ 1) for d in range(dp_count)]
    w_own = final_projection_matrix
    w_a = lax.ppermute(w_own, "dp", ring(1))
    w_b = lax.ppermute(w_own, "dp", ring(-1))

    q = mapped_probe_matrix[0]
    k = mapped_lookup_matrix[0]
    v = mapped_content_matrix[0]
    g = retention_preactivation[0]
    ex = lax.all_to_all(
        extra_shrinkage[0].reshape(sp_count, 1, TOK),
        "sp",
        split_axis=0,
        concat_axis=0,
        tiled=True,
    ).reshape(HEADS, TOK)
    qd, kd, p, bend = prep(q, k, g)
    u = update(ex, kd, v, bend)
    u_in = lax.all_to_all(u, "sp", split_axis=0, concat_axis=0, tiled=True)
    s = prefix(u_in)
    s_in = lax.all_to_all(s, "sp", split_axis=0, concat_axis=0, tiled=True)
    o_in = inside(ex, p, v)
    w_a2 = lax.ppermute(w_a, "dp", ring(1))

    head_out = heads(ex, qd, s_in, o_in, attention_group_scale.reshape(1, HEADS * DV))
    head_other = lax.ppermute(head_out, "dp", swap)

    sgn = 1 - 2 * core
    other = 1 - core
    y_up = (ychip + sgn) % ychips
    y_down = (ychip - sgn) % ychips
    y_far = (ychip + 2) % ychips
    place = jnp.stack(
        [
            ychip * 2 + core,
            y_down * 2 + core,
            y_up * 2 + core,
            y_far * 2 + core,
            ychip * 2 + other,
            y_up * 2 + other,
            y_down * 2 + other,
            y_far * 2 + other,
        ]
    ).astype(jnp.int32)
    e = early(head_out, head_other, [w_own, w_a, w_b])
    es = lax.ppermute(e[:, TOK:], "dp", swap)
    l = early(head_out, head_other, [w_a2])
    ls = lax.ppermute(l[:, TOK:], "dp", swap)
    chosen = assigned_specialists[0].reshape(-1)
    onehot = (chosen[:, None] == jnp.arange(total, dtype=jnp.int32)[None, :]).astype(jnp.int32)
    ranks = jnp.sum((jnp.cumsum(onehot, axis=0) - onehot) * onehot, axis=1)
    slots = chosen * CAP + ranks
    weights = dispatcher_logits[0]
    weights = (weights / jnp.sum(weights, axis=1, keepdims=True)).reshape(-1)

    residual, outgoing = route(
        place,
        slots,
        e,
        l,
        es,
        ls,
        skip_stream_entering[0],
        blender_branch_scale.reshape(1, D),
        specialist_prenormal_scale.reshape(1, D),
        total * CAP,
    )
    arrived = lax.all_to_all(
        outgoing.reshape(total, CAP, ROW, 128),
        ("sp", "dp"),
        split_axis=0,
        concat_axis=0,
        tiled=True,
    )
    result = experts(
        arrived.reshape(total * CAP, D),
        specialist_switch_matrix[0],
        specialist_expand_matrix[0],
        specialist_contract_matrix[0],
    )
    back = lax.all_to_all(
        result.reshape(total, CAP, ROW, 128),
        ("sp", "dp"),
        split_axis=0,
        concat_axis=0,
        tiled=True,
    ).reshape(total * CAP, ROW, 128)
    out = combine(slots, weights, back, residual, specialist_branch_scale.reshape(1, D))
    return out.reshape(1, TOK, D)


def solution(mesh):
    return jax.shard_map(
        layer,
        mesh=mesh,
        in_specs=(
            P("dp", "sp", None),
            P("dp", "sp", None),
            P("dp", "sp", None),
            P("dp", "sp", None),
            P("dp", "sp", None),
            P("dp", "sp", None),
            P(),
            P(None, "dp"),
            P(),
            P(),
            P(("sp", "dp"), None, None),
            P(("sp", "dp"), None, None),
            P(("sp", "dp"), None, None),
            P(),
            P("dp", "sp", None),
            P("dp", "sp", None),
        ),
        out_specs=P("dp", "sp", None),
        check_vma=False,
    )
```
